32 devices in a mesh: ep: 8 (over z, core), tp: 4 (over y, x).
Axes of the slice: x: 2, y: 2, z: 4, core: 2. Of those that a mesh axis runs over, the one named last changes fastest.
Arguments:
- mixer_rows: bfloat16 [2048, 2048], P('ep'), may hold values from -8 to 8
- mixer_gain: float32 [2048], replicated, may hold values from 0.1 to 1.9
- w_query: bfloat16 [2048, 1024], P(None, 'tp'), may hold values from -0.125 to 0.125
- w_key: bfloat16 [2048, 1024], P(None, 'tp'), may hold values from -0.125 to 0.125
- w_value: bfloat16 [2048, 1024], P(None, 'tp'), may hold values from -0.125 to 0.125
- key_shift: float32 [16, 2048], P('tp'), may hold values from -14 to 0
- w_out: bfloat16 [1024, 2048], P(None, 'tp'), may hold values from -0.75 to 0.75
- expert_rows: bfloat16 [1024, 2048], P('ep'), may hold values from -6 to 6
- expert_gain: float32 [2048], replicated, may hold values from 0.1 to 1.9
- routes: int32 [1024, 4], P('ep'), may hold values from 0 to 7, all different within a row; in each aligned block of 128 rows (0 to 127, 128 to 255, ...) at most 128 rows name the same one
- route_weight: float32 [1024, 4], P('ep'), may hold values from 0.05 to 0.6
- w_gate: bfloat16 [8, 2048, 2048], P('ep', None, 'tp'), may hold values from -0.25 to 0.25
- w_up: bfloat16 [8, 2048, 2048], P('ep', None, 'tp'), may hold values from -0.25 to 0.25
- w_down: bfloat16 [8, 2048, 2048], P('ep', None, 'tp'), may hold values from -0.0625 to 0.0625
Outputs:
- mixer_out: bfloat16 [2048, 2048], P('ep', 'tp')
- expert_out: bfloat16 [1024, 2048], P('ep', 'tp')
The draws below stay inside these ranges and needn't reach their ends.
Inputs may be any that keep to these rules, and one draw needn't show every extreme that they name: `routes`: each row names 4 different experts. In each aligned block of 128 rows no expert is named by more than 128 rows, and in every draw some block names some expert exactly 128 times.
All inputs are finite; a program needn't handle non-finite values.
Results may differ from the reference program's by a relative error of at most 0.0073.
Values may be sent and summed in bfloat16 or wider, within the bound.
No kernel may reach another device: no remote copies, remote signals or barrier semaphores. Data moves between devices by JAX's collectives and lax.ppermute only.
A program may use at most 64 MiB of HBM per device.

```python
import math
import jax
import jax.numpy as jnp
import numpy as np
from jax import lax

D = 2048
HEAD_TOTAL = 16
HEAD_DIM = 64
FF = 2048
TOPK = 4
TOKA_DEV = 256
TOKB_DEV = 128
SEQUENCE_TOKENS = 2048
TOKB = 1024
EXPERTS = 8
CAP = 128
N_EP = 8


def draw_mixer_rows(key, part):
    parallel_lanes = jax.random.split(key, 2)
    block_count = SEQUENCE_TOKENS // TOKA_DEV
    baseline = jax.random.normal(parallel_lanes[0], (SEQUENCE_TOKENS, D), jnp.float32)
    common = jax.random.normal(parallel_lanes[1], (block_count, D), jnp.float32)
    values = baseline + jnp.repeat(common, TOKA_DEV, axis=0)
    return jnp.clip(values, -8.0, 8.0).astype(jnp.bfloat16)


def draw_key_shift(key, part):
    parallel_lanes = jax.random.split(key, 7)
    block_count = SEQUENCE_TOKENS // TOKA_DEV
    fast_share = 0.5
    head_pick = jax.random.uniform(parallel_lanes[0], (HEAD_TOTAL, 1), jnp.float32)
    fast_span = jnp.exp(jax.random.uniform(parallel_lanes[1], (HEAD_TOTAL, 1), jnp.float32, 3.4, 4.6))
    slow_span = SEQUENCE_TOKENS * jax.random.uniform(parallel_lanes[2], (HEAD_TOTAL, 1), jnp.float32, 1.0, 2.0)
    baseline = -jnp.log(jnp.where(head_pick < fast_share, fast_span, slow_span))
    block_level = jax.random.uniform(parallel_lanes[3], (HEAD_TOTAL, block_count), jnp.float32, -0.7, 0.7)
    roughness = jax.random.uniform(parallel_lanes[4], (HEAD_TOTAL, SEQUENCE_TOKENS), jnp.float32, -0.5, 0.5)
    displaced_values = baseline + jnp.repeat(block_level, TOKA_DEV, axis=1) + roughness
    surge_selection = jax.random.uniform(parallel_lanes[5], (1, SEQUENCE_TOKENS), jnp.float32) < 4.0 / SEQUENCE_TOKENS
    surge_degree = jax.random.uniform(parallel_lanes[6], (HEAD_TOTAL, SEQUENCE_TOKENS), jnp.float32, -1.4, 0.0)
    return jnp.where(surge_selection, surge_degree, displaced_values).astype(jnp.float32)


def steps_of(own_key, extent, cuts, least, largest):
    loudness = 1.0
    for position, shards_of in cuts:
        draws = jax.random.uniform(jax.random.fold_in(jax.random.fold_in(own_key, 6), position), (shards_of,), jnp.float32, least / len(cuts), largest / len(cuts))
        loudness = loudness * jnp.repeat(jnp.exp(draws), extent[position] // shards_of).reshape((-1,) + (1,) * (len(extent) - 1 - position))
    return loudness


def shared_out(key, own, number, rows, number_of, top, reach, slope):
    sequence = jax.random.permutation(key, number_of)
    crowded, usual = shares(number_of, rows * top, reach, slope, True), shares(number_of, rows * top, reach, slope, False)
    places = jnp.arange(number_of)

    def named(lengths, turn):
        used = int((lengths > 0).sum())
        fixed = max(1, used // 4)
        passed = fixed + (places - fixed + turn * (used - fixed)) % max(1, number_of - fixed)
        return jnp.zeros((number_of,), jnp.int32).at[sequence[jnp.where(places < fixed, places, passed)]].set(jnp.asarray(lengths, jnp.int32))

    lengths = jnp.where(number % 4 == 0, named(crowded, number // 4), named(usual, number - number // 4 - 1))
    mixed = jax.random.permutation(jax.random.fold_in(own, 3), number_of)
    source_of, sink = mixed[0:number_of // 2 * 2:2], mixed[1:number_of // 2 * 2:2]
    slack = jnp.minimum(lengths[source_of] - 1, reach - lengths[sink]) // 2
    slack = jnp.where((source_of == sequence[0]) | (sink == sequence[0]) | (lengths[sink] == 0), 0, jnp.maximum(slack, 0))
    passed = jax.random.randint(jax.random.fold_in(own, 4), (number_of // 2,), 0, 1 << 20) % (slack + 1)
    lengths = lengths.at[source_of].add(-passed).at[sink].add(passed)
    labels = jnp.searchsorted(jnp.cumsum(lengths), jnp.arange(rows * top), side="right").astype(jnp.int32)
    grid = labels.reshape(top, rows).T
    grid = grid[jax.random.permutation(jax.random.fold_in(own, 1), rows)]
    turn = jax.random.randint(jax.random.fold_in(own, 2), (rows, 1), 0, top)
    return jnp.take_along_axis(grid, (jnp.arange(top)[None, :] + turn) % top, axis=1)


def shares(amount, total, reach, slope, full):
    portions = [(1 << 20) // math.isqrt(rank ** slope) + 1 for rank in range(1, amount + 1)]
    largest = reach if full else min(reach, max(-(-total // amount), total * portions[0] // sum(portions)))
    least = 1 if total - largest >= amount - 1 else 0
    holding, spare = [largest] + [least] * (amount - 1), total - largest - least * (amount - 1)
    while spare > 0:
        movable = [i for i in range(1, amount) if holding[i] < largest] or [i for i in range(1, amount) if holding[i] < reach]
        mass, left = sum([portions[i] for i in movable]), spare
        for i in movable:
            more = min(reach - holding[i], max(1, left * portions[i] // mass), spare)
            holding[i] = holding[i] + more
            spare = spare - more
    return np.array(holding)


def gaussian(key, extent, deviation, reach, cuts=(), held_as=jnp.bfloat16):
    array = deviation * jax.random.normal(key, extent, jnp.float32)
    if cuts:
        array = array * steps_of(key, extent, cuts, -0.22, 0.18)
    return jnp.clip(array, -reach, reach).astype(held_as)


def setup_inputs(seed: int = 0) -> dict:
    streams_of = jax.random.split(jax.random.key(seed), 15)
    mixer_rows = draw_mixer_rows(jax.random.fold_in(streams_of[14], 71), 0)
    mixer_gain = jnp.clip(1.0 + 0.18 * jax.random.normal(streams_of[1], (D,), jnp.float32), 0.1, 1.9)
    w_query = gaussian(streams_of[2], (D, HEAD_TOTAL * HEAD_DIM), D ** -0.5, 0.125, ((1, 4),))
    w_key = gaussian(streams_of[3], (D, HEAD_TOTAL * HEAD_DIM), D ** -0.5, 0.125, ((1, 4),))
    w_value = gaussian(streams_of[4], (D, HEAD_TOTAL * HEAD_DIM), D ** -0.5, 0.125, ((1, 4),))
    key_shift = draw_key_shift(jax.random.fold_in(streams_of[14], 71), 0)
    w_out = gaussian(streams_of[6], (HEAD_TOTAL * HEAD_DIM, D), (HEAD_TOTAL * HEAD_DIM // 16) ** -0.5, 0.75, ((1, 4),))
    expert_rows = gaussian(streams_of[7], (TOKB, D), 1.0, 6.0, ((0, 8),))
    expert_gain = jnp.clip(1.0 + 0.18 * jax.random.normal(streams_of[8], (D,), jnp.float32), 0.1, 1.9)
    routes_keys = jax.random.split(jax.random.fold_in(streams_of[9], 1), TOKB // TOKB_DEV)
    routes_turns = jax.random.permutation(jax.random.fold_in(streams_of[9], 3), TOKB // TOKB_DEV)
    routes = jax.vmap(lambda own, number: shared_out(jax.random.fold_in(streams_of[9], 2), own, number, TOKB_DEV, EXPERTS, TOPK, CAP, 2))(routes_keys, routes_turns).reshape((TOKB, TOPK))
    route_weight = jnp.clip(0.05 + 0.55 * jax.random.uniform(streams_of[10], (TOKB, TOPK), jnp.float32) ** steps_of(streams_of[10], (TOKB, TOPK), ((0, 8),), -0.2, 0.2), 0.05, 0.6)
    w_gate = gaussian(streams_of[11], (EXPERTS, D, FF), (D // 4) ** -0.5, 0.25, ((0, 8), (2, 4)))
    w_up = gaussian(streams_of[12], (EXPERTS, D, FF), (D // 4) ** -0.5, 0.25, ((0, 8), (2, 4)))
    w_down = gaussian(streams_of[13], (EXPERTS, FF, D), (4 * FF) ** -0.5, 0.0625, ((0, 8), (2, 4)))
    return {"mixer_rows": mixer_rows, "mixer_gain": mixer_gain, "w_query": w_query, "w_key": w_key, "w_value": w_value, "key_shift": key_shift, "w_out": w_out, "expert_rows": expert_rows, "expert_gain": expert_gain, "routes": routes, "route_weight": route_weight, "w_gate": w_gate, "w_up": w_up, "w_down": w_down}


norm_eps = 1e-06
glu_limit = 7.0
glu_alpha = 1.702

def rms_scale(source, scaling):
    floats = source.astype(jnp.float32)
    inverse = lax.rsqrt(lax.optimization_barrier(jnp.mean(floats * floats, axis=-1, keepdims=True)) + norm_eps)
    return (floats * inverse * scaling).astype(jnp.bfloat16)

def mixer_layer(mixer_rows, mixer_gain, w_query, w_key, w_value, key_shift, w_out):
    normed = rms_scale(mixer_rows, mixer_gain)
    total_rows = normed.shape[0]

    def project(weight):
        flat_out = jnp.dot(normed, weight, preferred_element_type=jnp.float32).astype(jnp.bfloat16)
        return flat_out.reshape(total_rows, HEAD_TOTAL, HEAD_DIM).transpose(1, 0, 2)
    positions = jnp.arange(total_rows, dtype=jnp.int32)
    block_starts = jnp.arange(total_rows // TOKA_DEV, dtype=jnp.int32) * TOKA_DEV

    def one_head(operands):
        query_head, key_head, value_head, shift_head = operands

        def one_block(begin_at):
            query_block = lax.dynamic_slice_in_dim(query_head, begin_at, TOKA_DEV, 0)
            query_pos = begin_at + jnp.arange(TOKA_DEV, dtype=jnp.int32)
            strict = positions[None, :] < query_pos[:, None]
            scores = jnp.dot(query_block, key_head.T, preferred_element_type=jnp.float32) * HEAD_DIM ** (-0.5)
            scores = scores + shift_head[None, :]
            log_stay = jnp.where(strict, jax.nn.log_sigmoid(-scores), 0.0)
            between = lax.cumsum(log_stay, axis=1, reverse=True) - log_stay
            weights = jnp.where(strict, jnp.exp(jax.nn.log_sigmoid(scores) + between), 0.0).astype(jnp.bfloat16)
            return jnp.dot(weights, value_head, preferred_element_type=jnp.float32).astype(jnp.bfloat16)
        return lax.map(one_block, block_starts).reshape(total_rows, HEAD_DIM)
    heads_out = lax.map(one_head, (project(w_query), project(w_key), project(w_value), key_shift))
    head_out = heads_out.transpose(1, 0, 2).reshape(total_rows, HEAD_TOTAL * HEAD_DIM)
    return jnp.dot(head_out, w_out, preferred_element_type=jnp.float32).astype(jnp.bfloat16)

def expert_layer(expert_rows, expert_gain, routes, route_weight, w_gate, w_up, w_down):
    normed = rms_scale(expert_rows, expert_gain)
    tokens_all = normed.shape[0]
    chosen = routes.reshape(-1).astype(jnp.int32)
    hit_table = (chosen[:, None] == jnp.arange(EXPERTS, dtype=jnp.int32)[None, :]).astype(jnp.int32)
    places = lax.optimization_barrier(jnp.sum((jnp.cumsum(hit_table, axis=0) - 1) * hit_table, axis=1)).astype(jnp.int32)
    room_size = N_EP * CAP
    targets = chosen * room_size + places
    assign_ids = jnp.arange(tokens_all * TOPK, dtype=jnp.int32) // TOPK
    owners = jnp.full((EXPERTS * room_size,), tokens_all, jnp.int32).at[targets].set(assign_ids)
    padded = jnp.concatenate([normed, jnp.zeros((1, D), jnp.bfloat16)], axis=0)

    def one_expert(operands):
        slot_ids, gate_cols, upper_cols, down_rows = operands
        picked_rows = padded[slot_ids]
        gating = jnp.minimum(jnp.dot(picked_rows, gate_cols, preferred_element_type=jnp.float32), glu_limit)
        linear = jnp.clip(jnp.dot(picked_rows, upper_cols, preferred_element_type=jnp.float32), -glu_limit, glu_limit)
        hidden = (gating * jax.nn.sigmoid(glu_alpha * gating) * (linear + 1.0)).astype(jnp.bfloat16)
        return jnp.dot(hidden, down_rows, preferred_element_type=jnp.float32).astype(jnp.bfloat16)
    results = lax.map(one_expert, (owners.reshape(EXPERTS, room_size), w_gate, w_up, w_down))
    picked = results.reshape(EXPERTS * room_size, D)[targets].astype(jnp.float32) * route_weight.reshape(-1)[:, None]
    return lax.optimization_barrier(jnp.sum(picked.reshape(tokens_all, TOPK, D), axis=1)).astype(jnp.bfloat16)

def reference(mixer_rows, mixer_gain, w_query, w_key, w_value, key_shift, w_out, expert_rows, expert_gain, routes, route_weight, w_gate, w_up, w_down):
    mixer_out = mixer_layer(mixer_rows, mixer_gain, w_query, w_key, w_value, key_shift, w_out)
    expert_out = expert_layer(expert_rows, expert_gain, routes, route_weight, w_gate, w_up, w_down)
    return (mixer_out, expert_out)
```

```python
import functools

import jax
import jax.numpy as jnp
from jax import lax
from jax.experimental import pallas as pl
from jax.experimental.pallas import tpu as pltpu
from jax.sharding import PartitionSpec as P

norm_eps = 1e-06
glu_limit = 7.0
glu_alpha = 1.702


def rms_scale(source, scaling):
    floats = source.astype(jnp.float32)
    inverse = lax.rsqrt(jnp.mean(floats * floats, axis=-1, keepdims=True) + norm_eps)
    return (floats * inverse * scaling).astype(jnp.bfloat16)


def stick_kernel(device_ref, q_ref, kv_ref, shift_ref, out_ref, acc_ref, carry_ref, *, head_count):
    length, columns = q_ref.shape
    width = columns // head_count
    device = device_ref[0]
    row = lax.broadcasted_iota(jnp.int32, (length, length), 0)
    col = lax.broadcasted_iota(jnp.int32, (length, length), 1)
    later = (row >= col).astype(jnp.bfloat16)
    strict = col < row
    scale = width ** (-0.5)

    def visit(block, first):
        start = pl.multiple_of(block * length, length)
        shifting = shift_ref[:, pl.ds(start, length)]
        for head in range(head_count):
            low, high = head * width, (head + 1) * width
            key_part = kv_ref[pl.ds(start, length), low:high]
            value_part = kv_ref[pl.ds(start, length), columns + low : columns + high]
            scores = lax.dot_general(
                q_ref[:, low:high],
                key_part,
                (((1,), (1,)), ((), ())),
                preferred_element_type=jnp.float32,
            )
            scores = scores * scale + shifting[head : head + 1, :]
            leave = jnp.maximum(scores, 0.0) + jnp.log(1.0 + jnp.exp(-jnp.abs(scores)))
            if first:
                leave = jnp.where(strict, leave, 0.0)
            coarse = leave.astype(jnp.bfloat16)
            fine = (leave - coarse.astype(jnp.float32)).astype(jnp.bfloat16)
            onward = jnp.dot(coarse, later, preferred_element_type=jnp.float32) + jnp.dot(
                fine, later, preferred_element_type=jnp.float32
            )
            if first:
                weights = jnp.where(strict, jnp.exp(scores - onward), 0.0)
                carry_ref[head] = onward[:, 0:1]
            else:
                carried = carry_ref[head]
                weights = jnp.exp(scores - onward - carried)
                carry_ref[head] = carried + onward[:, 0:1]
            contrib = jnp.dot(
                weights.astype(jnp.bfloat16), value_part, preferred_element_type=jnp.float32
            )
            if first:
                acc_ref[:, low:high] = contrib
            else:
                acc_ref[:, low:high] += contrib

    visit(device, True)

    @pl.loop(0, device)
    def _(step):
        visit(device - 1 - step, False)

    out_ref[...] = acc_ref[...].astype(jnp.bfloat16)


def stick_attention(device, queries, gathered, key_shift):
    length, columns = queries.shape
    head_count = key_shift.shape[0]
    vmem = pl.BlockSpec(memory_space=pltpu.VMEM)
    return pl.pallas_call(
        functools.partial(stick_kernel, head_count=head_count),
        in_specs=[pl.BlockSpec(memory_space=pltpu.SMEM), vmem, vmem, vmem],
        out_specs=vmem,
        out_shape=jax.ShapeDtypeStruct((length, columns), jnp.bfloat16),
        scratch_shapes=[
            pltpu.VMEM((length, columns), jnp.float32),
            pltpu.VMEM((head_count, length, 1), jnp.float32),
        ],
        cost_estimate=pl.CostEstimate(
            flops=8 * head_count * length * gathered.shape[0] * length,
            transcendentals=3 * head_count * length * gathered.shape[0],
            bytes_accessed=2 * gathered.size,
        ),
        name="stick_attention",
    )(device.reshape(1), queries, gathered, key_shift)


def per_device(
    mixer_rows,
    mixer_gain,
    w_query,
    w_key,
    w_value,
    key_shift,
    w_out,
    expert_rows,
    expert_gain,
    routes,
    route_weight,
    w_gate,
    w_up,
    w_down,
):
    tp_count = lax.axis_size("tp")
    ep_count = lax.axis_size("ep")
    tokens_here, top_count = routes.shape
    share = tokens_here // tp_count
    own_rows = lax.dynamic_slice_in_dim(expert_rows, lax.axis_index("tp") * share, share, 0)
    all_rows = lax.all_gather(
        rms_scale(own_rows, expert_gain), ("ep", "tp"), axis=0, tiled=True
    )

    normed = rms_scale(mixer_rows, mixer_gain)
    key_rows = jnp.dot(normed, w_key, preferred_element_type=jnp.float32).astype(jnp.bfloat16)
    value_rows = jnp.dot(normed, w_value, preferred_element_type=jnp.float32).astype(jnp.bfloat16)
    packed = jnp.concatenate([key_rows, value_rows], axis=1)
    gathered = lax.all_gather(packed, "ep", axis=0, tiled=True)
    queries = jnp.dot(normed, w_query, preferred_element_type=jnp.float32).astype(jnp.bfloat16)

    gating = jnp.minimum(
        jnp.dot(all_rows, w_gate[0], preferred_element_type=jnp.float32), glu_limit
    )
    linear = jnp.clip(
        jnp.dot(all_rows, w_up[0], preferred_element_type=jnp.float32), -glu_limit, glu_limit
    )
    hidden = (gating * jax.nn.sigmoid(glu_alpha * gating) * (linear + 1.0)).astype(jnp.bfloat16)
    units = lax.all_gather(hidden, "tp", axis=1, tiled=True)

    device = lax.axis_index("ep").astype(jnp.int32)
    head_out = stick_attention(device, queries, gathered, key_shift)
    mixer_out = jnp.dot(
        lax.all_gather(head_out, "tp", axis=1, tiled=True),
        w_out,
        preferred_element_type=jnp.float32,
    ).astype(jnp.bfloat16)

    results = jnp.dot(units, w_down[0], preferred_element_type=jnp.float32).astype(jnp.bfloat16)
    leaving = results.reshape(ep_count, tokens_here, results.shape[1])
    returned = lax.all_to_all(leaving, "ep", split_axis=0, concat_axis=0, tiled=True)
    named = routes[None] == jnp.arange(ep_count, dtype=jnp.int32)[:, None, None]
    shares = jnp.sum(jnp.where(named, route_weight[None], 0.0), axis=2)
    expert_out = jnp.sum(returned.astype(jnp.float32) * shares[:, :, None], axis=0).astype(
        jnp.bfloat16
    )
    return (mixer_out, expert_out)


def solution(mesh):
    placed = (
        P("ep", None),
        P(),
        P(None, "tp"),
        P(None, "tp"),
        P(None, "tp"),
        P("tp", None),
        P(None, "tp"),
        P("ep", None),
        P(),
        P("ep", None),
        P("ep", None),
        P("ep", None, "tp"),
        P("ep", None, "tp"),
        P("ep", None, "tp"),
    )
    return jax.shard_map(
        per_device,
        mesh=mesh,
        in_specs=placed,
        out_specs=(P("ep", "tp"), P("ep", "tp")),
        check_vma=False,
    )
```

```python
import functools

import jax
import jax.numpy as jnp
from jax import lax
from jax.experimental import pallas as pl
from jax.experimental.pallas import tpu as pltpu
from jax.sharding import PartitionSpec as P

norm_eps = 1e-06
glu_limit = 7.0
glu_alpha = 1.702


def rms_scale(source, scaling):
    floats = source.astype(jnp.float32)
    inverse = lax.rsqrt(jnp.mean(floats * floats, axis=-1, keepdims=True) + norm_eps)
    return (floats * inverse * scaling).astype(jnp.bfloat16)


def stick_kernel(device_ref, q_ref, kv_ref, shift_ref, out_ref, acc_ref, carry_ref, *, head_count):
    length, columns = q_ref.shape
    width = columns // head_count
    device = device_ref[0]
    row = lax.broadcasted_iota(jnp.int32, (length, length), 0)
    col = lax.broadcasted_iota(jnp.int32, (length, length), 1)
    later = (row >= col).astype(jnp.bfloat16)
    strict = col < row
    scale = width ** (-0.5)

    def visit(block, first):
        start = pl.multiple_of(block * length, length)
        place = block ^ device
        shifting = shift_ref[:, pl.ds(start, length)]
        for head in range(head_count):
            low, high = head * width, (head + 1) * width
            key_part = kv_ref[place, :, low:high]
            value_part = kv_ref[place, :, columns + low : columns + high]
            scores = lax.dot_general(
                q_ref[:, low:high],
                key_part,
                (((1,), (1,)), ((), ())),
                preferred_element_type=jnp.float32,
            )
            scores = scores * scale + shifting[head : head + 1, :]
            leave = jnp.maximum(scores, 0.0) + jnp.log(1.0 + jnp.exp(-jnp.abs(scores)))
            if first:
                leave = jnp.where(strict, leave, 0.0)
            coarse = leave.astype(jnp.bfloat16)
            fine = (leave - coarse.astype(jnp.float32)).astype(jnp.bfloat16)
            onward = jnp.dot(coarse, later, preferred_element_type=jnp.float32) + jnp.dot(
                fine, later, preferred_element_type=jnp.float32
            )
            if first:
                weights = jnp.where(strict, jnp.exp(scores - onward), 0.0)
                carry_ref[head] = onward[:, 0:1]
            else:
                carried = carry_ref[head]
                weights = jnp.exp(scores - onward - carried)
                carry_ref[head] = carried + onward[:, 0:1]
            contrib = jnp.dot(
                weights.astype(jnp.bfloat16), value_part, preferred_element_type=jnp.float32
            )
            if first:
                acc_ref[:, low:high] = contrib
            else:
                acc_ref[:, low:high] += contrib

    visit(device, True)

    @pl.loop(0, device)
    def _(step):
        visit(device - 1 - step, False)

    out_ref[...] = acc_ref[...].astype(jnp.bfloat16)


def stick_attention(device, queries, gathered, key_shift):
    length, columns = queries.shape
    head_count = key_shift.shape[0]
    vmem = pl.BlockSpec(memory_space=pltpu.VMEM)
    return pl.pallas_call(
        functools.partial(stick_kernel, head_count=head_count),
        in_specs=[pl.BlockSpec(memory_space=pltpu.SMEM), vmem, vmem, vmem],
        out_specs=vmem,
        out_shape=jax.ShapeDtypeStruct((length, columns), jnp.bfloat16),
        scratch_shapes=[
            pltpu.VMEM((length, columns), jnp.float32),
            pltpu.VMEM((head_count, length, 1), jnp.float32),
        ],
        cost_estimate=pl.CostEstimate(
            flops=8 * head_count * length * key_shift.shape[1] * length,
            transcendentals=3 * head_count * length * key_shift.shape[1],
            bytes_accessed=2 * gathered.size,
        ),
        name="stick_attention",
    )(device.reshape(1), queries, gathered, key_shift)


def flip(value, axis, mask):
    size = lax.axis_size(axis)
    return lax.ppermute(value, axis, [(place, place ^ mask) for place in range(size)])


def cube_gather(value, axis, backwards):
    size = lax.axis_size(axis)
    masks = [1 << bit for bit in range(size.bit_length() - 1)]
    items = {0: value}
    for mask in masks[::-1] if backwards else masks:
        for key in list(items):
            items[key ^ mask] = flip(items[key], axis, mask)
    return [items[key] for key in range(size)]


def per_device(
    mixer_rows,
    mixer_gain,
    w_query,
    w_key,
    w_value,
    key_shift,
    w_out,
    expert_rows,
    expert_gain,
    routes,
    route_weight,
    w_gate,
    w_up,
    w_down,
):
    tp_count = lax.axis_size("tp")
    ep_count = lax.axis_size("ep")
    line = ep_count // 2
    half = line // 2
    device = lax.axis_index("ep").astype(jnp.int32)
    column = lax.axis_index("tp").astype(jnp.int32)
    tokens_here, top_count = routes.shape
    share = tokens_here // tp_count

    def hidden_units(rows):
        gating = jnp.minimum(
            jnp.dot(rows, w_gate[0], preferred_element_type=jnp.float32), glu_limit
        )
        linear = jnp.clip(
            jnp.dot(rows, w_up[0], preferred_element_type=jnp.float32), -glu_limit, glu_limit
        )
        return (gating * jax.nn.sigmoid(glu_alpha * gating) * (linear + 1.0)).astype(jnp.bfloat16)

    own_rows = lax.dynamic_slice_in_dim(expert_rows, column * share, share, 0)
    own_rows = rms_scale(own_rows, expert_gain)
    along = [own_rows] + [flip(own_rows, "ep", 2 * step) for step in range(1, line)]
    groups = [
        cube_gather(jnp.concatenate(along[:half], axis=0), "tp", False),
        cube_gather(jnp.concatenate(along[half:], axis=0), "tp", True),
    ]
    near_rows = jnp.zeros((tp_count, line * share, own_rows.shape[1]), jnp.bfloat16)
    for number, group in enumerate(groups):
        for key, piece in enumerate(group):
            near_rows = lax.dynamic_update_slice(
                near_rows, piece[None], (column ^ key, number * half * share, 0)
            )
    near_rows = near_rows.reshape(tp_count * line * share, own_rows.shape[1])
    far_rows = flip(near_rows, "ep", 1)

    named = routes[None] == jnp.arange(ep_count, dtype=jnp.int32)[:, None, None]
    shares = jnp.sum(jnp.where(named, route_weight[None], 0.0), axis=2)
    scales = lax.all_to_all(shares, "ep", split_axis=0, concat_axis=0, tiled=True)
    scales = scales[jnp.arange(ep_count, dtype=jnp.int32) ^ device]
    scales = scales.reshape(line, 2, tp_count, share).transpose(1, 2, 0, 3)

    normed = rms_scale(mixer_rows, mixer_gain)
    key_rows = jnp.dot(normed, w_key, preferred_element_type=jnp.float32).astype(jnp.bfloat16)
    value_rows = jnp.dot(normed, w_value, preferred_element_type=jnp.float32).astype(jnp.bfloat16)
    packed = jnp.concatenate([key_rows, value_rows], axis=1)
    keys_along = [packed] + [flip(packed, "ep", 2 * step) for step in range(1, line)]
    queries = jnp.dot(normed, w_query, preferred_element_type=jnp.float32).astype(jnp.bfloat16)
    near_hidden = hidden_units(near_rows)
    _, keys_along = lax.optimization_barrier((near_hidden, keys_along))
    near_keys = jnp.stack(keys_along, axis=0)
    far_keys = flip(near_keys, "ep", 1)
    gathered = jnp.stack([near_keys, far_keys], axis=1).reshape(ep_count, *packed.shape)

    def spread(block):
        middle = block.shape[0] // 2
        first = cube_gather(block[:middle], "tp", False)
        second = cube_gather(block[middle:], "tp", True)
        return [jnp.concatenate(pair, axis=0) for pair in zip(first, second)]

    def contract(pieces, weight):
        depth = weight.shape[0] // tp_count
        total = None
        for key, piece in enumerate(pieces):
            rows = lax.dynamic_slice_in_dim(weight, (column ^ key) * depth, depth, 0)
            part = jnp.dot(piece, rows, preferred_element_type=jnp.float32)
            total = part if total is None else total + part
        return total

    near_units = spread(near_hidden)
    far_hidden = hidden_units(far_rows)
    _, queries, down_rows = lax.optimization_barrier((far_hidden, queries, w_down[0]))
    far_units = spread(far_hidden)

    head_out = stick_attention(device, queries, gathered, key_shift)
    mixer_out = contract(spread(head_out), w_out).astype(jnp.bfloat16)

    def weighted(units, scale):
        results = contract(units, down_rows)
        return results.reshape(*scale.shape, results.shape[1]) * scale[..., None]

    far_sum = weighted(far_units, scales[1]).astype(jnp.bfloat16)
    near_sum = weighted(near_units, scales[0])
    near_sum = near_sum + flip(far_sum, "ep", 1).astype(jnp.float32)
    total = near_sum[:, 0]
    for step in range(1, line):
        total = total + flip(near_sum[:, step].astype(jnp.bfloat16), "ep", 2 * step).astype(
            jnp.float32
        )
    expert_out = total.reshape(tokens_here, total.shape[2]).astype(jnp.bfloat16)
    return (mixer_out, expert_out)


def solution(mesh):
    placed = (
        P("ep", None),
        P(),
        P(None, "tp"),
        P(None, "tp"),
        P(None, "tp"),
        P("tp", None),
        P(None, "tp"),
        P("ep", None),
        P(),
        P("ep", None),
        P("ep", None),
        P("ep", None, "tp"),
        P("ep", None, "tp"),
        P("ep", None, "tp"),
    )
    return jax.shard_map(
        per_device,
        mesh=mesh,
        in_specs=placed,
        out_specs=(P("ep", "tp"), P("ep", "tp")),
        check_vma=False,
    )
```
